32 devices in a mesh: fs: 8 (over z, y), tp: 4 (over x, core).
Axes of the slice: x: 2, y: 2, z: 4, core: 2. Of those that a mesh axis runs over, the one named last changes fastest.
Arguments:
- tokens: bfloat16 [4096, 2048], P(('fs', 'tp')), may hold values from -6 to 6
- pre_gain: float32 [2048], replicated, may hold values from 0.1 to 1.9
- w_expand: bfloat16 [2048, 8192], P('fs', 'tp'), may hold values from -0.125 to 0.125
- w_reduce: bfloat16 [8192, 2048], P('tp', 'fs'), may hold values from -0.0625 to 0.0625
- post_gain: float32 [2048], replicated, may hold values from 0.1 to 1.9
Outputs:
- result: bfloat16 [4096, 2048], P(('fs', 'tp'))
The draws below stay inside these ranges and needn't reach their ends.
All inputs are finite; a program needn't handle non-finite values.
Results may differ from the reference program's by a relative error of at most 0.014.
Values may be sent and summed in bfloat16 or wider, within the bound.
A program may use at most 64 MiB of HBM per device.

```python
import math
import jax
import jax.numpy as jnp
from jax import lax

D = 2048
FF = 8192
TOKENS = 4096
N_TP = 4


def block_levels(key, shape, cuts, low, top_value):
    level, own = 1.0, jax.random.fold_in(key, 6)
    for dim, parts in cuts:
        draws = jnp.exp(jax.random.uniform(jax.random.fold_in(own, dim), (parts,), jnp.float32, low / len(cuts), top_value / len(cuts)))
        level = level * jnp.repeat(draws, shape[dim] // parts).reshape([-1 if axis == dim else 1 for axis in range(len(shape))])
    return level


def centred(key, extent, deviation, reach, shards=(), held_as=jnp.bfloat16):
    drawn = jax.random.normal(key, extent, jnp.float32) * deviation
    if len(shards) > 0:
        drawn = block_levels(key, extent, shards, -0.22, 0.18) * drawn
    return jnp.clip(drawn, min=-reach, max=reach).astype(held_as)


def setup_inputs(seed: int = 0) -> dict:
    key_list = jax.random.split(jax.random.key(seed), 6)
    return {
        "tokens": centred(key_list[0], (TOKENS, D), 1.0, 6.0, ((0, 32),)),
        "pre_gain": jnp.clip(1.0 + 0.18 * jax.random.normal(key_list[1], (D,), jnp.float32), 0.1, 1.9),
        "w_expand": centred(key_list[2], (D, FF), D ** -0.5, 0.125, ((0, 8), (1, 4))),
        "w_reduce": centred(key_list[3], (FF, D), FF ** -0.5, 0.0625, ((0, 4), (1, 8))),
        "post_gain": jnp.clip(1.0 + 0.18 * jax.random.normal(key_list[4], (D,), jnp.float32), 0.1, 1.9),
    }


NORM_EPS = 1e-06

def rms_scale(values, gain_row):
    widened = values.astype(jnp.float32)
    scaled = widened * lax.rsqrt(lax.optimization_barrier(jnp.mean(widened * widened, axis=-1, keepdims=True)) + NORM_EPS)
    return scaled * gain_row.astype(jnp.float32)

def reference(tokens, pre_gain, w_expand, w_reduce, post_gain):
    row_count = tokens.shape[0]
    block_rows = math.gcd(row_count, 2048)
    blocks = tokens.reshape(row_count // block_rows, block_rows, D)
    hidden_block = FF // N_TP

    def per_block(block):
        normed = rms_scale(block, pre_gain).astype(jnp.bfloat16)
        preact = jnp.dot(normed, w_expand, preferred_element_type=jnp.float32)
        hidden = jnp.square(jnp.maximum(preact, 0.0)).astype(jnp.bfloat16)
        running = jnp.zeros((block_rows, D), jnp.float32)
        for member in range(N_TP):
            partial_value = jnp.dot(hidden[:, member * hidden_block:(member + 1) * hidden_block], w_reduce[member * hidden_block:(member + 1) * hidden_block], preferred_element_type=jnp.float32).astype(jnp.bfloat16)
            partial_value = lax.optimization_barrier(partial_value)
            running = running + partial_value.astype(jnp.float32)
        mixed = running.astype(jnp.bfloat16)
        return rms_scale(mixed, post_gain).astype(jnp.bfloat16)
    return lax.map(per_block, blocks).reshape(row_count, D)
```

```python
import functools
import math

import jax
import jax.numpy as jnp
from jax import lax
from jax.experimental import pallas as pl
from jax.experimental.pallas import tpu as pltpu
from jax.sharding import PartitionSpec as P

NORM_EPS = 1e-06
MESH = pl.DeviceIdType.MESH


def kernel(NX, NY, NZ, tok, gain_in, w_e, w_r, gain_out, out,
           TG, N, WE, WR, H, O, PR, RX,
           t_ls, t_ps, t_r, e_a, e_b, e_c, e_r, r_a, r_b, r_c, r_r, p_s, p_r, c_s, c_r):
    R, D = tok.shape
    DK, F = w_e.shape
    H4 = F // NZ
    fs, tp = lax.axis_index("fs"), lax.axis_index("tp")
    z, y = fs // NY, fs % NY
    x, c = tp // 2, tp % 2
    pc = 1 - c
    peer = (fs, x * 2 + pc)

    def zdev(q):
        return (q * NY + y, tp)

    xs = [(x + j) % NX for j in range(1, NX)]
    ys = [(y + j) % NY for j in range(1, NY)]
    xdevs = [(fs, q * 2 + c) for q in xs]
    ydevs = [(z * NY + q, tp) for q in ys]

    barrier = pltpu.get_barrier_semaphore()
    others = [zdev((z + j) % NZ) for j in range(1, NZ)] + xdevs + ydevs + [peer]
    for dev in others:
        pl.semaphore_signal(barrier, inc=1, device_id=dev, device_id_type=MESH)
    pl.semaphore_wait(barrier, len(others))

    def rc(src, dst, ss, rs, dev):
        return pltpu.make_async_remote_copy(src_ref=src, dst_ref=dst, send_sem=ss, recv_sem=rs,
                                            device_id=dev, device_id_type=MESH)

    sent = []

    def go(cond, make):
        if cond is None:
            make().start()
        else:
            pl.when(cond)(lambda: make().start())
        sent.append((cond, make))

    def guarded(cond, fn):
        if cond is None:
            fn()
        else:
            pl.when(cond)(fn)

    def at_distance(d):
        if d == 0:
            return [(z, 0, None)]
        return [(z - d, -1, z - d >= 0), (z + d, 1, z + d < NZ)]

    def e_view(xq, zq, yq):
        return WE.at[xq, pl.ds(pl.multiple_of((zq * NY + yq) * DK, DK), DK)]

    def r_view(xq, zq, yq):
        return WR.at[zq * NY + yq, pl.ds(pl.multiple_of(xq * H4, H4), H4)]

    def e_piece(q):
        return w_e.at[:, pl.ds(pl.multiple_of(q * H4, H4), H4)]

    def r_piece(q):
        return w_r.at[pl.ds(pl.multiple_of(q * H4, H4), H4)]

    own = [
        pltpu.make_async_copy(tok, TG.at[z, c], t_r.at[z, c]),
        pltpu.make_async_copy(e_piece(z), e_view(x, z, y), e_r.at[x, z, y]),
        pltpu.make_async_copy(r_piece(z), r_view(x, z, y), r_r.at[x, z, y]),
    ]
    for copy in own:
        copy.start()
    for side, (q, ok) in enumerate(((z - 1, z >= 1), (z + 1, z + 1 < NZ))):
        go(ok, lambda q=q, side=side: rc(tok, TG.at[z, c], t_ls.at[z, side], t_r.at[z, c], zdev(q)))
    go(None, lambda: rc(tok, TG.at[z, c], t_ps.at[z], t_r.at[z, c], peer))
    for view, piece, a_s, r in ((e_view, e_piece, e_a, e_r), (r_view, r_piece, r_a, r_r)):
        for d in range(1, NZ):
            for q, s, ok in at_distance(d):
                go(ok, lambda q=q, view=view, piece=piece, a_s=a_s, r=r:
                   rc(piece(q), view(x, z, y), a_s.at[q], r.at[x, z, y], zdev(q)))

    def landed(ref, sem):
        pltpu.make_async_copy(ref, ref, sem).wait()

    def tokens_step(d):
        for q, s, ok in at_distance(d):
            guarded(ok, lambda q=q: landed(TG.at[q, c], t_r.at[q, c]))
            if d > 0:
                n = z - s
                go(jnp.logical_and(ok, jnp.logical_and(n >= 0, n < NZ)),
                   lambda q=q, n=n, s=s: rc(TG.at[q, c], TG.at[q, c], t_ls.at[q, (1 - s) // 2],
                                            t_r.at[q, c], zdev(n)))
                go(ok, lambda q=q: rc(TG.at[q, c], TG.at[q, c], t_ps.at[q], t_r.at[q, c], peer))

    def first_step(d, view, r, b_s, c_s_, x_first):
        for q, s, ok in at_distance(d):
            guarded(ok, lambda q=q: landed(view(x, q, y), r.at[x, q, y]))
            firsts, lasts = (xdevs, ydevs) if x_first else (ydevs, xdevs)
            for j, dev in enumerate(firsts):
                go(ok, lambda q=q, j=j, dev=dev: rc(view(x, q, y), view(x, q, y), b_s.at[q, j],
                                                    r.at[x, q, y], dev))
            for j, dev in enumerate(lasts):
                go(ok, lambda q=q, j=j, dev=dev: rc(view(x, q, y), view(x, q, y), c_s_.at[q, 0, j],
                                                    r.at[x, q, y], dev))

    def second_step(d, view, r, c_s_, x_first):
        for q, s, ok in at_distance(d):
            for i, m in enumerate(xs if x_first else ys):
                where = (m, q, y) if x_first else (x, q, m)
                guarded(ok, lambda where=where: landed(view(*where), r.at[where]))
                for j, dev in enumerate(ydevs if x_first else xdevs):
                    go(ok, lambda q=q, i=i, j=j, dev=dev, where=where:
                       rc(view(*where), view(*where), c_s_.at[q, 1 + i, j], r.at[where], dev))

    def last_step(d, view, r, x_first):
        for q, s, ok in at_distance(d):
            for a in [x] + xs if x_first else xs:
                for b in ys if x_first else [y] + ys:
                    guarded(ok, lambda q=q, a=a, b=b: landed(view(a, q, b), r.at[a, q, b]))

    def normalize():
        for q in range(NZ):
            landed(TG.at[q, pc], t_r.at[q, pc])
        sub = 32

        def body(i, carry):
            b, row = i // (R // sub), (i % (R // sub)) * sub
            row = pl.multiple_of(row, sub)
            v = TG[b // 2, b % 2, pl.ds(row, sub)].astype(jnp.float32)
            v = v * lax.rsqrt(jnp.mean(v * v, axis=-1, keepdims=True) + NORM_EPS) * gain_in[...]
            N[pl.ds(pl.multiple_of(i * sub, sub), sub)] = v.astype(jnp.bfloat16)
            return carry

        lax.fori_loop(0, NZ * 2 * R // sub, body, 0)

    rows = NZ * 2 * R
    MB = math.gcd(4, NZ * 2)
    M = MB * R

    def expand():
        def body(i, carry):
            xq, row = i // (rows // M), pl.multiple_of((i % (rows // M)) * M, M)
            p = jnp.dot(N[pl.ds(row, M)], WE[xq], preferred_element_type=jnp.float32)
            H[xq, pl.ds(row, M)] = jnp.square(jnp.maximum(p, 0.0)).astype(jnp.bfloat16)
            return carry

        lax.fori_loop(0, NX * (rows // M), body, 0)

    def reduce_column(f):
        def body(i, carry):
            row = pl.multiple_of(i * M, M)
            p = jnp.dot(H[0, pl.ds(row, M)], WR[f, :H4], preferred_element_type=jnp.float32)
            for xq in range(1, NX):
                p += jnp.dot(H[xq, pl.ds(row, M)], WR[f, xq * H4:(xq + 1) * H4],
                             preferred_element_type=jnp.float32)
            O[pl.ds(i * MB, MB), f] = p.astype(jnp.bfloat16).reshape(MB, R, DK)
            return carry

        lax.fori_loop(0, rows // M, body, 0)

    for d in range(NZ):
        tokens_step(d)
        first_step(d, e_view, e_r, e_b, e_c, True)
        if d > 0:
            second_step(d - 1, e_view, e_r, e_c, True)
    second_step(NZ - 1, e_view, e_r, e_c, True)
    for d in range(NZ):
        first_step(d, r_view, r_r, r_b, r_c, False)
        if d > 0:
            second_step(d - 1, r_view, r_r, r_c, False)
        if d == NZ - 2:
            normalize()
            for k in range(NZ):
                last_step(k, e_view, e_r, True)
            expand()
    second_step(NZ - 1, r_view, r_r, r_c, False)
    for d in range(NZ):
        last_step(d, r_view, r_r, False)
    lax.fori_loop(0, NZ * NY, lambda f, carry: (reduce_column(f), carry)[1], 0)

    for k in range(NZ):
        go(None, lambda k=k: rc(O.at[k * 2 + pc], PR.at[k], p_s.at[k], p_r.at[k], peer))

    def add_block(q, slots):
        def body(f, carry):
            s = O[q * 2 + c, f].astype(jnp.float32) + PR[q, f].astype(jnp.float32)
            for slot in slots:
                s += RX[slot, f].astype(jnp.float32)
            O[q * 2 + c, f] = s.astype(jnp.bfloat16)
            return carry

        lax.fori_loop(0, NZ * NY, body, 0)

    for k in range(NZ):
        landed(PR.at[k], p_r.at[k])

    for j in range(NZ - 1):
        for q, n, ok, has in ((NZ - 1 - j, z + 1, NZ - 1 - j > z, z > 0), (j, z - 1, j < z, z < NZ - 1)):
            inner = jnp.logical_and(ok, has)

            def with_arrived(q=q):
                landed(RX.at[q], c_r.at[q])
                add_block(q, [q])

            pl.when(inner)(with_arrived)
            pl.when(jnp.logical_and(ok, jnp.logical_not(has)))(lambda q=q: add_block(q, []))
            slot = jnp.where(jnp.logical_and(n < z, n == q), NZ, q)
            go(ok, lambda q=q, n=n, slot=slot: rc(O.at[q * 2 + c], RX.at[slot], c_s.at[q], c_r.at[slot], zdev(n)))

    pl.when(z > 0)(lambda: landed(RX.at[z], c_r.at[z]))
    pl.when(z < NZ - 1)(lambda: landed(RX.at[NZ], c_r.at[NZ]))
    pl.when(jnp.logical_and(z > 0, z < NZ - 1))(lambda: add_block(z, [z, NZ]))
    pl.when(z == 0)(lambda: add_block(z, [NZ]))
    pl.when(z == NZ - 1)(lambda: add_block(z, [z]))

    def squares(f, acc):
        m = O[z * 2 + c, f].astype(jnp.float32)
        return acc + jnp.sum(m * m, axis=-1, keepdims=True)

    total = lax.fori_loop(0, NZ * NY, squares, jnp.zeros((R, 1), jnp.float32))
    scale = lax.rsqrt(total / D + NORM_EPS)
    for f in range(NZ * NY):
        cols = slice(f * DK, (f + 1) * DK)
        out[:, cols] = (O[z * 2 + c, f].astype(jnp.float32) * scale * gain_out[:, cols]).astype(jnp.bfloat16)

    for cond, make in sent:
        guarded(cond, lambda make=make: make().wait_send())


def per_device(FS, TP, tokens, pre_gain, w_expand, w_reduce, post_gain):
    NX = TP // 2
    NY = max(k for k in range(1, FS + 1) if FS % k == 0 and (k == 1 or 2 * k * k <= FS))
    NZ = FS // NY
    R, D = tokens.shape
    DK, F = w_expand.shape
    H4 = F // NZ
    rows = NZ * 2 * R
    bf = jnp.bfloat16
    dma = pltpu.SemaphoreType.DMA
    mx = max(NX, NY)
    vmem = pl.BlockSpec(memory_space=pltpu.VMEM)
    hbm = pl.BlockSpec(memory_space=pl.ANY)
    return pl.pallas_call(
        functools.partial(kernel, NX, NY, NZ),
        out_shape=jax.ShapeDtypeStruct((R, D), bf),
        in_specs=[hbm, vmem, hbm, hbm, vmem],
        out_specs=vmem,
        scratch_shapes=[
            pltpu.VMEM((NZ, 2, R, D), bf),
            pltpu.VMEM((rows, D), bf),
            pltpu.VMEM((NX, D, H4), bf),
            pltpu.VMEM((FS, NX * H4, DK), bf),
            pltpu.VMEM((NX, rows, H4), bf),
            pltpu.VMEM((NZ * 2, FS, R, DK), bf),
            pltpu.VMEM((NZ, FS, R, DK), bf),
            pltpu.VMEM((NZ + 1, FS, R, DK), bf),
            dma((NZ, 2)), dma((NZ,)), dma((NZ, 2)),
            dma((NZ,)), dma((NZ, mx)), dma((NZ, mx, mx)), dma((NX, NZ, NY)),
            dma((NZ,)), dma((NZ, mx)), dma((NZ, mx, mx)), dma((NX, NZ, NY)),
            dma((NZ,)), dma((NZ,)), dma((NZ,)), dma((NZ + 1,)),
        ],
        compiler_params=pltpu.CompilerParams(
            collective_id=0, has_side_effects=True, vmem_limit_bytes=64 * 1024 * 1024 - 128 * 1024),
    )(tokens, pre_gain.reshape(1, D), w_expand, w_reduce, post_gain.reshape(1, D))


def solution(mesh):
    return jax.shard_map(
        functools.partial(per_device, mesh.shape["fs"], mesh.shape["tp"]),
        mesh=mesh,
        in_specs=(P(("fs", "tp"), None), P(), P("fs", "tp"), P("tp", "fs"), P()),
        out_specs=P(("fs", "tp"), None),
        check_vma=False,
    )
```

```python
import functools

import jax
import jax.numpy as jnp
from jax import lax
from jax.experimental import pallas as pl
from jax.experimental.pallas import tpu as pltpu
from jax.sharding import PartitionSpec as P

NORM_EPS = 1e-06
MESH = pl.DeviceIdType.MESH


def kernel(NX, NY, NZ, tok, gain_in, w_e, w_r, gain_out, out,
           TG, N, WE, WR, H, O, PR, RX,
           t_ls, t_ps, t_r, e_a, e_b, e_c, e_l, e_r, r_a, r_b, r_c, r_l, r_r, p_s, p_r, c_s, c_r):
    R, D = tok.shape
    DK, F = w_e.shape
    H4 = F // NZ
    fs, tp = lax.axis_index("fs"), lax.axis_index("tp")
    z, y = fs // NY, fs % NY
    x, c = tp // 2, tp % 2
    pc = 1 - c
    peer = (fs, x * 2 + pc)

    def zdev(q):
        return (q * NY + y, tp)

    xs = [(x + j) % NX for j in range(1, NX)]
    ys = [(y + j) % NY for j in range(1, NY)]
    xdevs = [(fs, q * 2 + c) for q in xs]
    ydevs = [(z * NY + q, tp) for q in ys]

    barrier = pltpu.get_barrier_semaphore()
    others = [zdev((z + j) % NZ) for j in range(1, NZ)] + xdevs + ydevs + [peer]
    for dev in others:
        pl.semaphore_signal(barrier, inc=1, device_id=dev, device_id_type=MESH)
    pl.semaphore_wait(barrier, len(others))

    def rc(src, dst, ss, rs, dev):
        return pltpu.make_async_remote_copy(src_ref=src, dst_ref=dst, send_sem=ss, recv_sem=rs,
                                            device_id=dev, device_id_type=MESH)

    sent = []

    def go(cond, make):
        if cond is None:
            make().start()
        else:
            pl.when(cond)(lambda: make().start())
        sent.append((cond, make))

    def guarded(cond, fn):
        if cond is None:
            fn()
        else:
            pl.when(cond)(fn)

    def at_distance(d):
        if d == 0:
            return [(z, 0, None)]
        return [(z - d, -1, z - d >= 0), (z + d, 1, z + d < NZ)]

    def rows_of(start, size, half):
        if half is None:
            return pl.ds(pl.multiple_of(start, size), size)
        return pl.ds(pl.multiple_of(start + half * (size // 2), size // 2), size // 2)

    def e_view(xq, zq, yq, half=None):
        return WE.at[xq, rows_of((zq * NY + yq) * DK, DK, half)]

    def r_view(xq, zq, yq, half=None):
        return WR.at[zq * NY + yq, rows_of(xq * H4, H4, half)]

    def e_piece(q):
        return w_e.at[:, pl.ds(pl.multiple_of(q * H4, H4), H4)]

    def r_piece(q):
        return w_r.at[pl.ds(pl.multiple_of(q * H4, H4), H4)]

    own = [
        pltpu.make_async_copy(tok, TG.at[z, c], t_r.at[z, c]),
        pltpu.make_async_copy(e_piece(z), e_view(x, z, y), e_l.at[z]),
        pltpu.make_async_copy(r_piece(z), r_view(x, z, y), r_l.at[z]),
    ]
    for copy in own:
        copy.start()
    def line_pieces(view, piece, a_s, r):
        for d in range(1, NZ):
            for q, s, ok in at_distance(d):
                go(ok, lambda q=q: rc(piece(q), view(x, z, y), a_s.at[q], r.at[z], zdev(q)))

    def own_tokens():
        for side, (q, ok) in enumerate(((z - 1, z >= 1), (z + 1, z + 1 < NZ))):
            go(ok, lambda q=q, side=side: rc(tok, TG.at[z, c], t_ls.at[z, side], t_r.at[z, c], zdev(q)))
        go(None, lambda: rc(tok, TG.at[z, c], t_ps.at[z], t_r.at[z, c], peer))

    line_pieces(e_view, e_piece, e_a, e_l)
    own_tokens()
    line_pieces(r_view, r_piece, r_a, r_l)

    def landed(ref, sem):
        pltpu.make_async_copy(ref, ref, sem).wait()

    def tokens_step(d):
        for q, s, ok in at_distance(d):
            guarded(ok, lambda q=q: landed(TG.at[q, c], t_r.at[q, c]))
            if d > 0:
                n = z - s
                go(jnp.logical_and(ok, jnp.logical_and(n >= 0, n < NZ)),
                   lambda q=q, n=n, s=s: rc(TG.at[q, c], TG.at[q, c], t_ls.at[q, (1 - s) // 2],
                                            t_r.at[q, c], zdev(n)))
                go(ok, lambda q=q: rc(TG.at[q, c], TG.at[q, c], t_ps.at[q], t_r.at[q, c], peer))

    ways = ((xdevs, xs, ydevs, ys), (ydevs, ys, xdevs, xs))

    def first_step(d, view, l, r, b_s, c_s_):
        for q, s, ok in at_distance(d):
            guarded(ok, lambda q=q: landed(view(x, q, y), l.at[q]))
            for h in (0, 1):
                for j, dev in enumerate(ways[h][0]):
                    go(ok, lambda q=q, j=j, dev=dev, h=h: rc(view(x, q, y, h), view(x, q, y, h), b_s.at[q, j, h],
                                                             r.at[x, q, y, h], dev))
            for h in (0, 1):
                for j, dev in enumerate(ways[h][2]):
                    go(ok, lambda q=q, j=j, dev=dev, h=h: rc(view(x, q, y, h), view(x, q, y, h), c_s_.at[q, 0, j, h],
                                                             r.at[x, q, y, h], dev))

    def second_step(d, view, r, c_s_):
        for q, s, ok in at_distance(d):
            for h in (0, 1):
                for i, m in enumerate(ways[h][1]):
                    where = (m, q, y) if h == 0 else (x, q, m)
                    guarded(ok, lambda where=where, h=h: landed(view(*where, h), r.at[(*where, h)]))
                    for j, dev in enumerate(ways[h][2]):
                        go(ok, lambda q=q, i=i, j=j, dev=dev, where=where, h=h:
                           rc(view(*where, h), view(*where, h), c_s_.at[q, 1 + i, j, h], r.at[(*where, h)], dev))

    def last_step(d, view, r):
        for q, s, ok in at_distance(d):
            for h in (0, 1):
                for a in [x] + xs if h == 0 else xs:
                    for b in ys if h == 0 else [y] + ys:
                        guarded(ok, lambda a=a, b=b, q=q, h=h: landed(view(a, q, b, h), r.at[a, q, b, h]))

    M = 2 * R
    sub = 32

    def rows_step(q):
        landed(TG.at[q, pc], t_r.at[q, pc])

        def norm(i, carry):
            v = TG[q, i // (R // sub), pl.ds(pl.multiple_of((i % (R // sub)) * sub, sub), sub)].astype(jnp.float32)
            v = v * lax.rsqrt(jnp.mean(v * v, axis=-1, keepdims=True) + NORM_EPS) * gain_in[...]
            N[pl.ds(pl.multiple_of(i * sub, sub), sub)] = v.astype(jnp.bfloat16)
            return carry

        lax.fori_loop(0, M // sub, norm, 0)

        def expand(i, carry):
            p = jnp.dot(N[...], WE[i], preferred_element_type=jnp.float32)
            H[i] = jnp.square(jnp.maximum(p, 0.0)).astype(jnp.bfloat16)
            return carry

        lax.fori_loop(0, NX, expand, 0)

        def column(f, carry):
            p = jnp.dot(H[0], WR[f, :H4], preferred_element_type=jnp.float32)
            for xq in range(1, NX):
                p += jnp.dot(H[xq], WR[f, xq * H4:(xq + 1) * H4], preferred_element_type=jnp.float32)
            O[pl.ds(q * 2, 2), f] = p.astype(jnp.bfloat16).reshape(2, R, DK)
            return carry

        lax.fori_loop(0, NZ * NY, column, 0)

    tokens_step(0)
    for d in range(NZ):
        first_step(d, e_view, e_l, e_r, e_b, e_c)
        if d == 0:
            first_step(d, r_view, r_l, r_r, r_b, r_c)
        if d > 0:
            second_step(d - 1, e_view, e_r, e_c)
        if d == NZ - 1:
            tokens_step(1)
    second_step(NZ - 1, e_view, e_r, e_c)
    second_step(0, r_view, r_r, r_c)
    for d in range(1, NZ):
        first_step(d, r_view, r_l, r_r, r_b, r_c)
        if d > 1:
            second_step(d - 1, r_view, r_r, r_c)
            tokens_step(d)
    second_step(NZ - 1, r_view, r_r, r_c)
    for d in range(NZ):
        last_step(d, e_view, e_r)
        last_step(d, r_view, r_r)
    for d in range(NZ):
        for q, s, ok in at_distance(d):
            guarded(ok, lambda q=q: rows_step(q))
            go(ok, lambda q=q: rc(O.at[q * 2 + pc], PR.at[q], p_s.at[q], p_r.at[q], peer))

    def add_block(q, slots):
        def body(f, carry):
            s = O[q * 2 + c, f].astype(jnp.float32) + PR[q, f].astype(jnp.float32)
            for slot in slots:
                s += RX[slot, f].astype(jnp.float32)
            O[q * 2 + c, f] = s.astype(jnp.bfloat16)
            return carry

        lax.fori_loop(0, NZ * NY, body, 0)

    for k in range(NZ):
        landed(PR.at[k], p_r.at[k])

    for j in range(NZ - 1):
        for q, n, ok, has in ((NZ - 1 - j, z + 1, NZ - 1 - j > z, z > 0), (j, z - 1, j < z, z < NZ - 1)):
            inner = jnp.logical_and(ok, has)

            def with_arrived(q=q):
                landed(RX.at[q], c_r.at[q])
                add_block(q, [q])

            pl.when(inner)(with_arrived)
            pl.when(jnp.logical_and(ok, jnp.logical_not(has)))(lambda q=q: add_block(q, []))
            slot = jnp.where(jnp.logical_and(n < z, n == q), NZ, q)
            go(ok, lambda q=q, n=n, slot=slot: rc(O.at[q * 2 + c], RX.at[slot], c_s.at[q], c_r.at[slot], zdev(n)))

    pl.when(z > 0)(lambda: landed(RX.at[z], c_r.at[z]))
    pl.when(z < NZ - 1)(lambda: landed(RX.at[NZ], c_r.at[NZ]))
    pl.when(jnp.logical_and(z > 0, z < NZ - 1))(lambda: add_block(z, [z, NZ]))
    pl.when(z == 0)(lambda: add_block(z, [NZ]))
    pl.when(z == NZ - 1)(lambda: add_block(z, [z]))

    def squares(f, acc):
        m = O[z * 2 + c, f].astype(jnp.float32)
        return acc + jnp.sum(m * m, axis=-1, keepdims=True)

    total = lax.fori_loop(0, NZ * NY, squares, jnp.zeros((R, 1), jnp.float32))
    scale = lax.rsqrt(total / D + NORM_EPS)
    for f in range(NZ * NY):
        cols = slice(f * DK, (f + 1) * DK)
        out[:, cols] = (O[z * 2 + c, f].astype(jnp.float32) * scale * gain_out[:, cols]).astype(jnp.bfloat16)

    for cond, make in sent:
        guarded(cond, lambda make=make: make().wait_send())


def per_device(FS, TP, tokens, pre_gain, w_expand, w_reduce, post_gain):
    NX = TP // 2
    NY = max(k for k in range(1, FS + 1) if FS % k == 0 and (k == 1 or 2 * k * k <= FS))
    NZ = FS // NY
    R, D = tokens.shape
    DK, F = w_expand.shape
    H4 = F // NZ
    bf = jnp.bfloat16
    dma = pltpu.SemaphoreType.DMA
    mx = max(NX, NY)
    vmem = pl.BlockSpec(memory_space=pltpu.VMEM)
    hbm = pl.BlockSpec(memory_space=pl.ANY)
    return pl.pallas_call(
        functools.partial(kernel, NX, NY, NZ),
        out_shape=jax.ShapeDtypeStruct((R, D), bf),
        in_specs=[hbm, vmem, hbm, hbm, vmem],
        out_specs=vmem,
        scratch_shapes=[
            pltpu.VMEM((NZ, 2, R, D), bf),
            pltpu.VMEM((2 * R, D), bf),
            pltpu.VMEM((NX, D, H4), bf),
            pltpu.VMEM((FS, NX * H4, DK), bf),
            pltpu.VMEM((NX, 2 * R, H4), bf),
            pltpu.VMEM((NZ * 2, FS, R, DK), bf),
            pltpu.VMEM((NZ, FS, R, DK), bf),
            pltpu.VMEM((NZ + 1, FS, R, DK), bf),
            dma((NZ, 2)), dma((NZ,)), dma((NZ, 2)),
            dma((NZ,)), dma((NZ, mx, 2)), dma((NZ, mx, mx, 2)), dma((NZ,)), dma((NX, NZ, NY, 2)),
            dma((NZ,)), dma((NZ, mx, 2)), dma((NZ, mx, mx, 2)), dma((NZ,)), dma((NX, NZ, NY, 2)),
            dma((NZ,)), dma((NZ,)), dma((NZ,)), dma((NZ + 1,)),
        ],
        compiler_params=pltpu.CompilerParams(
            collective_id=0, has_side_effects=True, vmem_limit_bytes=64 * 1024 * 1024 - 128 * 1024),
    )(tokens, pre_gain.reshape(1, D), w_expand, w_reduce, post_gain.reshape(1, D))


def solution(mesh):
    return jax.shard_map(
        functools.partial(per_device, mesh.shape["fs"], mesh.shape["tp"]),
        mesh=mesh,
        in_specs=(P(("fs", "tp"), None), P(), P("fs", "tp"), P("tp", "fs"), P()),
        out_specs=P(("fs", "tp"), None),
        check_vma=False,
    )
```

```python
import functools

import jax
import jax.numpy as jnp
from jax import lax
from jax.experimental import pallas as pl
from jax.experimental.pallas import tpu as pltpu
from jax.sharding import PartitionSpec as P

NORM_EPS = 1e-06
MESH = pl.DeviceIdType.MESH


def kernel(NX, NY, NZ, tok, gain_in, w_e, w_r, gain_out, out,
           TG, N, WE, WR, H, O, PR, RX,
           t_ls, t_ps, t_r, e_a, e_b, e_c, e_l, e_r, r_a, r_b, r_c, r_l, r_r, p_s, p_r, c_s, c_r):
    R, D = tok.shape
    DK, F = w_e.shape
    H4 = F // NZ
    fs, tp = lax.axis_index("fs"), lax.axis_index("tp")
    z, y = fs // NY, fs % NY
    x, c = tp // 2, tp % 2
    pc = 1 - c
    peer = (fs, x * 2 + pc)

    def zdev(q):
        return (q * NY + y, tp)

    xs = [(x + j) % NX for j in range(1, NX)]
    ys = [(y + j) % NY for j in range(1, NY)]
    xdevs = [(fs, q * 2 + c) for q in xs]
    ydevs = [(z * NY + q, tp) for q in ys]

    barrier = pltpu.get_barrier_semaphore()
    others = [zdev((z + j) % NZ) for j in range(1, NZ)] + xdevs + ydevs + [peer]
    for dev in others:
        pl.semaphore_signal(barrier, inc=1, device_id=dev, device_id_type=MESH)
    pl.semaphore_wait(barrier, len(others))

    def rc(src, dst, ss, rs, dev):
        return pltpu.make_async_remote_copy(src_ref=src, dst_ref=dst, send_sem=ss, recv_sem=rs,
                                            device_id=dev, device_id_type=MESH)

    sent = []

    def go(cond, make):
        if cond is None:
            make().start()
        else:
            pl.when(cond)(lambda: make().start())
        sent.append((cond, make))

    def guarded(cond, fn):
        if cond is None:
            fn()
        else:
            pl.when(cond)(fn)

    def at_distance(d):
        if d == 0:
            return [(z, 0, None)]
        return [(z - d, -1, z - d >= 0), (z + d, 1, z + d < NZ)]

    def rows_of(start, size, half):
        if half is None:
            return pl.ds(pl.multiple_of(start, size), size)
        return pl.ds(pl.multiple_of(start + half * (size // 2), size // 2), size // 2)

    def e_view(xq, zq, yq, half=None):
        return WE.at[xq, rows_of((zq * NY + yq) * DK, DK, half)]

    def r_view(xq, zq, yq, half=None):
        return WR.at[zq * NY + yq, rows_of(xq * H4, H4, half)]

    def e_piece(q):
        return w_e.at[:, pl.ds(pl.multiple_of(q * H4, H4), H4)]

    def r_piece(q):
        return w_r.at[pl.ds(pl.multiple_of(q * H4, H4), H4)]

    own = [
        pltpu.make_async_copy(tok, TG.at[z, c], t_r.at[z, c]),
        pltpu.make_async_copy(e_piece(z), e_view(x, z, y), e_l.at[z]),
        pltpu.make_async_copy(r_piece(z), r_view(x, z, y), r_l.at[z]),
    ]
    for copy in own:
        copy.start()
    def line_pieces(view, piece, a_s, r):
        for d in range(1, NZ):
            for q, s, ok in at_distance(d):
                go(ok, lambda q=q: rc(piece(q), view(x, z, y), a_s.at[q], r.at[z], zdev(q)))

    def own_tokens():
        for side, (q, ok) in enumerate(((z - 1, z >= 1), (z + 1, z + 1 < NZ))):
            go(ok, lambda q=q, side=side: rc(tok, TG.at[z, c], t_ls.at[z, side], t_r.at[z, c], zdev(q)))
        go(None, lambda: rc(tok, TG.at[z, c], t_ps.at[z], t_r.at[z, c], peer))

    line_pieces(e_view, e_piece, e_a, e_l)
    own_tokens()
    line_pieces(r_view, r_piece, r_a, r_l)

    def landed(ref, sem):
        pltpu.make_async_copy(ref, ref, sem).wait()

    def tokens_step(d):
        for q, s, ok in at_distance(d):
            guarded(ok, lambda q=q: landed(TG.at[q, c], t_r.at[q, c]))
            if d > 0:
                n = z - s
                go(jnp.logical_and(ok, jnp.logical_and(n >= 0, n < NZ)),
                   lambda q=q, n=n, s=s: rc(TG.at[q, c], TG.at[q, c], t_ls.at[q, (1 - s) // 2],
                                            t_r.at[q, c], zdev(n)))
                go(ok, lambda q=q: rc(TG.at[q, c], TG.at[q, c], t_ps.at[q], t_r.at[q, c], peer))

    ways = ((xdevs, xs, ydevs, ys), (ydevs, ys, xdevs, xs))

    def first_step(d, view, l, r, b_s, c_s_):
        for q, s, ok in at_distance(d):
            guarded(ok, lambda q=q: landed(view(x, q, y), l.at[q]))
            for h in (0, 1):
                for j, dev in enumerate(ways[h][0]):
                    go(ok, lambda q=q, j=j, dev=dev, h=h: rc(view(x, q, y, h), view(x, q, y, h), b_s.at[q, j, h],
                                                             r.at[x, q, y, h], dev))
            for h in (0, 1):
                for j, dev in enumerate(ways[h][2]):
                    go(ok, lambda q=q, j=j, dev=dev, h=h: rc(view(x, q, y, h), view(x, q, y, h), c_s_.at[q, 0, j, h],
                                                             r.at[x, q, y, h], dev))

    def second_step(d, view, r, c_s_):
        for q, s, ok in at_distance(d):
            for h in (0, 1):
                for i, m in enumerate(ways[h][1]):
                    where = (m, q, y) if h == 0 else (x, q, m)
                    guarded(ok, lambda where=where, h=h: landed(view(*where, h), r.at[(*where, h)]))
                    for j, dev in enumerate(ways[h][2]):
                        go(ok, lambda q=q, i=i, j=j, dev=dev, where=where, h=h:
                           rc(view(*where, h), view(*where, h), c_s_.at[q, 1 + i, j, h], r.at[(*where, h)], dev))

    def last_step(d, view, r):
        for q, s, ok in at_distance(d):
            for h in (0, 1):
                for a in [x] + xs if h == 0 else xs:
                    for b in ys if h == 0 else [y] + ys:
                        guarded(ok, lambda a=a, b=b, q=q, h=h: landed(view(a, q, b, h), r.at[a, q, b, h]))

    M = 2 * R
    sub = 32

    def expand_rows(q):
        landed(TG.at[q, pc], t_r.at[q, pc])

        def norm(i, carry):
            v = TG[q, i // (R // sub), pl.ds(pl.multiple_of((i % (R // sub)) * sub, sub), sub)].astype(jnp.float32)
            v = v * lax.rsqrt(jnp.mean(v * v, axis=-1, keepdims=True) + NORM_EPS) * gain_in[...]
            N[pl.ds(pl.multiple_of(i * sub, sub), sub)] = v.astype(jnp.bfloat16)
            return carry

        lax.fori_loop(0, M // sub, norm, 0)

        def expand(i, carry):
            p = jnp.dot(N[...], WE[i], preferred_element_type=jnp.float32)
            H[i, pl.ds(pl.multiple_of(q * M, M), M)] = jnp.square(jnp.maximum(p, 0.0)).astype(jnp.bfloat16)
            return carry

        lax.fori_loop(0, NX, expand, 0)

    big = 2 * M if NZ % 2 == 0 else M

    def columns(q):
        def body(k, carry):
            f, i = q * NY + k // (NZ * M // big), k % (NZ * M // big)
            row = pl.ds(pl.multiple_of(i * big, big), big)
            p = jnp.dot(H[0, row], WR[f, :H4], preferred_element_type=jnp.float32)
            for xq in range(1, NX):
                p += jnp.dot(H[xq, row], WR[f, xq * H4:(xq + 1) * H4], preferred_element_type=jnp.float32)
            O[pl.ds(i * (big // R), big // R), f] = p.astype(jnp.bfloat16).reshape(big // R, R, DK)
            return carry

        lax.fori_loop(0, NY * NZ * M // big, body, 0)

    tokens_step(0)
    for d in range(NZ):
        first_step(d, e_view, e_l, e_r, e_b, e_c)
        if d == 0:
            first_step(d, r_view, r_l, r_r, r_b, r_c)
        if d > 0:
            second_step(d - 1, e_view, e_r, e_c)
        if d == NZ - 1:
            tokens_step(1)
    second_step(NZ - 1, e_view, e_r, e_c)
    second_step(0, r_view, r_r, r_c)
    for d in range(1, NZ):
        first_step(d, r_view, r_l, r_r, r_b, r_c)
        if d > 1:
            second_step(d - 1, r_view, r_r, r_c)
            tokens_step(d)
    for d in range(NZ):
        last_step(d, e_view, e_r)

    def expand_at(d):
        for q, s, ok in at_distance(d):
            guarded(ok, lambda q=q: expand_rows(q))

    expand_at(0)
    expand_at(1)
    second_step(NZ - 1, r_view, r_r, r_c)
    for d in range(2, NZ):
        expand_at(d)
    for d in range(NZ):
        last_step(d, r_view, r_r)
        for q, s, ok in at_distance(d):
            guarded(ok, lambda q=q: columns(q))

    FH = NZ * NY // 2

    def part(h):
        return pl.ds(h * FH, FH)

    order = []
    for k in range((NZ + 1) // 2):
        order += [NZ - 1 - k] + ([k] if k != NZ - 1 - k else [])
    for h in (0, 1):
        for q in order:
            go(None, lambda q=q, h=h: rc(O.at[q * 2 + pc, part(h)], PR.at[q, part(h)], p_s.at[q, h], p_r.at[q, h], peer))

    def add_part(q, h, slots):
        landed(PR.at[q, part(h)], p_r.at[q, h])
        for slot in slots:
            landed(RX.at[slot, part(h)], c_r.at[slot, h])

        def body(f, carry):
            s = O[q * 2 + c, f].astype(jnp.float32) + PR[q, f].astype(jnp.float32)
            for slot in slots:
                s += RX[slot, f].astype(jnp.float32)
            O[q * 2 + c, f] = s.astype(jnp.bfloat16)
            return carry

        lax.fori_loop(h * FH, (h + 1) * FH, body, 0)

    for j in range(NZ - 1):
        for h in (0, 1):
            for q, n, ok, has in ((NZ - 1 - j, z + 1, NZ - 1 - j > z, z > 0), (j, z - 1, j < z, z < NZ - 1)):
                pl.when(jnp.logical_and(ok, has))(lambda q=q, h=h: add_part(q, h, [q]))
                pl.when(jnp.logical_and(ok, jnp.logical_not(has)))(lambda q=q, h=h: add_part(q, h, []))
                slot = jnp.where(jnp.logical_and(n < z, n == q), NZ, q)
                go(ok, lambda q=q, n=n, slot=slot, h=h: rc(O.at[q * 2 + c, part(h)], RX.at[slot, part(h)],
                                                           c_s.at[q, h], c_r.at[slot, h], zdev(n)))
    for h in (0, 1):
        pl.when(jnp.logical_and(z > 0, z < NZ - 1))(lambda h=h: add_part(z, h, [z, NZ]))
        pl.when(z == 0)(lambda h=h: add_part(z, h, [NZ]))
        pl.when(z == NZ - 1)(lambda h=h: add_part(z, h, [z]))

    def squares(f, acc):
        m = O[z * 2 + c, f].astype(jnp.float32)
        return acc + jnp.sum(m * m, axis=-1, keepdims=True)

    total = lax.fori_loop(0, NZ * NY, squares, jnp.zeros((R, 1), jnp.float32))
    scale = lax.rsqrt(total / D + NORM_EPS)
    for f in range(NZ * NY):
        cols = slice(f * DK, (f + 1) * DK)
        out[:, cols] = (O[z * 2 + c, f].astype(jnp.float32) * scale * gain_out[:, cols]).astype(jnp.bfloat16)

    for cond, make in sent:
        guarded(cond, lambda make=make: make().wait_send())


def per_device(FS, TP, tokens, pre_gain, w_expand, w_reduce, post_gain):
    NX = TP // 2
    NY = max(k for k in range(1, FS + 1) if FS % k == 0 and (k == 1 or 2 * k * k <= FS))
    NZ = FS // NY
    R, D = tokens.shape
    DK, F = w_expand.shape
    H4 = F // NZ
    bf = jnp.bfloat16
    dma = pltpu.SemaphoreType.DMA
    mx = max(NX, NY)
    vmem = pl.BlockSpec(memory_space=pltpu.VMEM)
    hbm = pl.BlockSpec(memory_space=pl.ANY)
    return pl.pallas_call(
        functools.partial(kernel, NX, NY, NZ),
        out_shape=jax.ShapeDtypeStruct((R, D), bf),
        in_specs=[hbm, vmem, hbm, hbm, vmem],
        out_specs=vmem,
        scratch_shapes=[
            pltpu.VMEM((NZ, 2, R, D), bf),
            pltpu.VMEM((2 * R, D), bf),
            pltpu.VMEM((NX, D, H4), bf),
            pltpu.VMEM((FS, NX * H4, DK), bf),
            pltpu.VMEM((NX, NZ * 2 * R, H4), bf),
            pltpu.VMEM((NZ * 2, FS, R, DK), bf),
            pltpu.VMEM((NZ, FS, R, DK), bf),
            pltpu.VMEM((NZ + 1, FS, R, DK), bf),
            dma((NZ, 2)), dma((NZ,)), dma((NZ, 2)),
            dma((NZ,)), dma((NZ, mx, 2)), dma((NZ, mx, mx, 2)), dma((NZ,)), dma((NX, NZ, NY, 2)),
            dma((NZ,)), dma((NZ, mx, 2)), dma((NZ, mx, mx, 2)), dma((NZ,)), dma((NX, NZ, NY, 2)),
            dma((NZ, 2)), dma((NZ, 2)), dma((NZ, 2)), dma((NZ + 1, 2)),
        ],
        compiler_params=pltpu.CompilerParams(
            collective_id=0, has_side_effects=True, vmem_limit_bytes=64 * 1024 * 1024 - 128 * 1024),
    )(tokens, pre_gain.reshape(1, D), w_expand, w_reduce, post_gain.reshape(1, D))


def solution(mesh):
    return jax.shard_map(
        functools.partial(per_device, mesh.shape["fs"], mesh.shape["tp"]),
        mesh=mesh,
        in_specs=(P(("fs", "tp"), None), P(), P("fs", "tp"), P("tp", "fs"), P()),
        out_specs=P(("fs", "tp"), None),
        check_vma=False,
    )
```
